32 devices in a mesh: kv: 8 (over z, y), tp: 4 (over x, core).
Axes of the slice: x: 2, y: 2, z: 4, core: 2. Of those that a mesh axis runs over, the one named last changes fastest.
Arguments:
- piece_tokens: bfloat16 [768, 4096], P('kv'), may hold values from -6 to 6
- step_tokens: bfloat16 [8, 4096], P('kv'), may hold values from -6 to 6
- in_gain: float32 [4096], replicated, may hold values from 0.1 to 1.9
- w_query: bfloat16 [4096, 8, 2, 128], P(None, 'tp'), may hold values from -0.09375 to 0.09375
- w_key: bfloat16 [4096, 8, 2, 128], P(None, 'tp'), may hold values from -0.15625 to 0.15625
- w_value: bfloat16 [4096, 8, 256], P(None, 'tp'), may hold values from -0.09375 to 0.09375
- w_out: bfloat16 [8, 256, 4096], P('tp'), may hold values from -0.125 to 0.125
- mix_ratio: float32 [8], P('tp'), may hold values from 0.3 to 0.8
- out_gain: float32 [256], replicated, may hold values from 0.1 to 1.9
- prompt_keys: bfloat16 [16384, 8, 2, 128], P('kv', 'tp'), may hold values from -630 to 630
- prompt_values: bfloat16 [16384, 8, 256], P('kv', 'tp'), may hold values from -6 to 6
- step_cache_keys: bfloat16 [8, 1024, 8, 2, 128], P(None, 'kv', 'tp'), may hold values from -630 to 630
- step_cache_values: bfloat16 [8, 1024, 8, 256], P(None, 'kv', 'tp'), may hold values from -6 to 6
- prompt_len: int32 [1], replicated, may hold values from 15360 to 16384
- step_lens: int32 [8], replicated, may hold values from 960 to 1024
Outputs:
- piece_out: bfloat16 [768, 4096], P('kv', 'tp')
- step_out: bfloat16 [8, 4096], P('kv', 'tp')
- piece_keys: bfloat16 [768, 8, 2, 128], P('kv', 'tp')
- piece_values: bfloat16 [768, 8, 256], P('kv', 'tp')
- step_keys: bfloat16 [8, 8, 2, 128], P('kv', 'tp')
- step_values: bfloat16 [8, 8, 256], P('kv', 'tp')
The draws below stay inside these ranges and needn't reach their ends.
Inputs may be any that keep to these rules, and one draw needn't show every extreme that they name: `prompt_len`: the piece's tokens follow these cached positions. `step_lens`: each decoding token follows its sequence's cached positions.
All inputs are finite; a program needn't handle non-finite values.
Results may differ from the reference program's by a relative error of at most 0.015.
Values may be sent and summed in bfloat16 or wider, within the bound.
A program may use at most 128 MiB of HBM per device.

```python
import jax
import jax.numpy as jnp
from jax import lax

D = 4096
HEADS = 8
DH = 128
DV = 256
PIECE_DEV = 96
PCAP_DEV = 2048
DEC_DEV = 1
DCAP_DEV = 128
PIECE = 768
PCAP = 16384
SEQS = 8
DEC_LEN = 1024
N_KV = 8
N_TP = 4


KEY_SCALE = 1.75


def base_keys(key, shape):
    return jnp.clip(jax.random.normal(key, shape, jnp.float32), -6.0, 6.0) * KEY_SCALE


def draw_prompt_keys(key, part):
    entries = base_keys(jax.random.fold_in(key, 3), (PCAP, HEADS, 2, DH))
    return entries.astype(jnp.bfloat16)


def draw_step_cache_keys(key, part):
    entries = base_keys(jax.random.fold_in(key, 7), (SEQS, DEC_LEN, HEADS, 2, DH))
    return entries.astype(jnp.bfloat16)


def touch_ends(array, own_key, smallest, top_value):
    longest = array.shape.index(max(array.shape))
    spots = []
    for shift in (0, 1):
        where = [jax.random.randint(jax.random.fold_in(own_key, axis), (), 0, length) for axis, length in enumerate(array.shape)]
        where[longest] = (where[longest] + shift) % array.shape[longest]
        spots.append(tuple(where))
    return array.at[spots[0]].set(smallest).at[spots[1]].set(top_value)


def block_levels(own_key, extent, pieces, low, high):
    gain = 1.0
    for dim, blocks in pieces:
        steps = jax.random.uniform(jax.random.fold_in(jax.random.fold_in(own_key, 6), dim), (blocks,), jnp.float32, low / len(pieces), high / len(pieces))
        gain = gain * jnp.repeat(jnp.exp(steps), extent[dim] // blocks).reshape((-1,) + (1,) * (len(extent) - 1 - dim))
    return gain


def noise(stream_key, dims, spread, limit, cuts=(), kind=jnp.bfloat16):
    values = spread * jax.random.normal(stream_key, dims, jnp.float32)
    if cuts:
        values = values * block_levels(stream_key, dims, cuts, -0.22, 0.18)
    return jnp.clip(values, -limit, limit).astype(kind)


def setup_inputs(seed: int = 0) -> dict:
    key_of = jax.random.split(jax.random.key(seed), 16)
    return {
        "piece_tokens": noise(key_of[0], (PIECE, D), 1.0, 6.0, ((0, 8),)),
        "step_tokens": noise(key_of[1], (SEQS, D), 1.0, 6.0, ((0, 8),)),
        "in_gain": jnp.clip(1.0 + 0.18 * jax.random.normal(key_of[2], (D,), jnp.float32), 0.1, 1.9),
        "w_query": noise(key_of[3], (D, HEADS, 2, DH), D ** -0.5, 0.09375, ((1, 4),)),
        "w_key": noise(key_of[4], (D, HEADS, 2, DH), (D // 3) ** -0.5, 0.15625, ((1, 4),)),
        "w_value": noise(key_of[5], (D, HEADS, DV), D ** -0.5, 0.09375, ((1, 4),)),
        "w_out": noise(key_of[6], (HEADS, DV, D), (HEADS * DV) ** -0.5, 0.125, ((0, 4),)),
        "mix_ratio": jnp.clip(0.3 + 0.5 * jax.random.uniform(key_of[7], (HEADS,), jnp.float32) ** block_levels(key_of[7], (HEADS,), ((0, 4),), -0.2, 0.2), 0.3, 0.8),
        "out_gain": jnp.clip(1.0 + 0.18 * jax.random.normal(key_of[8], (DV,), jnp.float32), 0.1, 1.9),
        "prompt_keys": draw_prompt_keys(jax.random.fold_in(key_of[15], 71), 0),
        "prompt_values": noise(key_of[10], (PCAP, HEADS, DV), 1.0, 6.0, ((0, 8), (1, 4))),
        "step_cache_keys": draw_step_cache_keys(jax.random.fold_in(key_of[15], 71), 0),
        "step_cache_values": noise(key_of[12], (SEQS, DEC_LEN, HEADS, DV), 1.0, 6.0, ((1, 8), (2, 4))),
        "prompt_len": jax.random.randint(key_of[13], (1,), PCAP - PCAP_DEV // 2, PCAP + 1).astype(jnp.int32),
        "step_lens": touch_ends(jax.random.randint(key_of[14], (SEQS,), DEC_LEN - DCAP_DEV // 2, DEC_LEN + 1), jax.random.fold_in(key_of[14], 1), DEC_LEN - DCAP_DEV // 2, DEC_LEN).astype(jnp.int32),
    }


EPS = 1e-06
OUT_SCALE = 0.8

def norm_rows(tokens, in_gain):
    floats = tokens.astype(jnp.float32)
    inv_rms = lax.rsqrt(lax.optimization_barrier(jnp.mean(floats * floats, axis=-1, keepdims=True)) + EPS)
    return (floats * inv_rms * in_gain.astype(jnp.float32)).astype(jnp.bfloat16)

def project(normed, weight):
    flat_weight = weight.reshape(weight.shape[0], -1)
    product = jnp.dot(normed, flat_weight, preferred_element_type=jnp.float32)
    rounded = lax.optimization_barrier(product.astype(jnp.bfloat16))
    return rounded.reshape((normed.shape[0],) + weight.shape[1:])

def head_partial(queries, key_rows, value_rows, visible):
    scores = jnp.einsum('qcd,kcd->cqk', queries.astype(jnp.float32), key_rows.astype(jnp.float32))
    scores = scores * queries.shape[-1] ** (-0.5)
    scores = jnp.where(visible[None], scores, -jnp.inf)
    maxima = lax.optimization_barrier(jnp.max(scores, axis=-1))
    weights = jnp.exp(scores - maxima[..., None])
    totals = lax.optimization_barrier(jnp.sum(weights, axis=-1))
    rounded = lax.optimization_barrier(weights.astype(jnp.bfloat16))
    summed = jnp.einsum('cqk,kv->qcv', rounded.astype(jnp.float32), value_rows.astype(jnp.float32))
    summed = lax.optimization_barrier(summed.astype(jnp.bfloat16))
    return (summed, jnp.transpose(maxima), jnp.transpose(totals))

def fold_group(running, summed, maxima, totals):
    row_best, norm_sum, value_sum = running
    new_best = jnp.maximum(row_best, maxima)
    old_scale = jnp.exp(row_best - new_best)
    new_scale = jnp.exp(maxima - new_best)
    return (new_best, norm_sum * old_scale + totals * new_scale, value_sum * old_scale[..., None] + summed.astype(jnp.float32) * new_scale[..., None])

def finish(norm_sum, value_sum, mix_ratio, out_gain):
    attended = value_sum / norm_sum[..., None]
    mixed = attended[:, :, 0] - mix_ratio[None, :, None] * attended[:, :, 1]
    inv_rms = lax.rsqrt(lax.optimization_barrier(jnp.mean(mixed * mixed, axis=-1, keepdims=True)) + EPS)
    return (mixed * inv_rms * out_gain[None, None, :] * OUT_SCALE).astype(jnp.bfloat16)

def empty_state(row_count):
    return (jnp.full((row_count, HEADS, 2), -jnp.inf, jnp.float32), jnp.zeros((row_count, HEADS, 2), jnp.float32), jnp.zeros((row_count, HEADS, 2, DV), jnp.float32))

def reference(piece_tokens, step_tokens, in_gain, w_query, w_key, w_value, w_out, mix_ratio, out_gain, prompt_keys, prompt_values, step_cache_keys, step_cache_values, prompt_len, step_lens):
    all_rows = jnp.concatenate([piece_tokens, step_tokens], axis=0)
    normed = norm_rows(all_rows, in_gain)
    queries = project(normed, w_query)
    key_rows = project(normed, w_key)
    value_rows = project(normed, w_value)
    piece_q = queries[:PIECE]
    step_q = queries[PIECE:]
    piece_k = key_rows[:PIECE]
    step_k = key_rows[PIECE:]
    piece_v = value_rows[:PIECE]
    step_v = value_rows[PIECE:]
    row_place = jnp.arange(PIECE, dtype=jnp.int32)
    seq_place = jnp.arange(SEQS, dtype=jnp.int32)

    def piece_group(running, group_id):
        cache_k = lax.dynamic_slice_in_dim(prompt_keys, group_id * PCAP_DEV, PCAP_DEV, 0)
        cache_v = lax.dynamic_slice_in_dim(prompt_values, group_id * PCAP_DEV, PCAP_DEV, 0)
        fresh_k = lax.dynamic_slice_in_dim(piece_k, group_id * PIECE_DEV, PIECE_DEV, 0)
        fresh_v = lax.dynamic_slice_in_dim(piece_v, group_id * PIECE_DEV, PIECE_DEV, 0)
        all_k = jnp.concatenate([cache_k, fresh_k], axis=0)
        all_v = jnp.concatenate([cache_v, fresh_v], axis=0)
        cache_place = group_id * PCAP_DEV + jnp.arange(PCAP_DEV, dtype=jnp.int32)
        fresh_place = group_id * PIECE_DEV + jnp.arange(PIECE_DEV, dtype=jnp.int32)
        visible = jnp.concatenate([jnp.broadcast_to((cache_place < prompt_len[0])[None, :], (PIECE, PCAP_DEV)), fresh_place[None, :] <= row_place[:, None]], axis=1)

        def one_head(operands):
            return head_partial(operands[0], operands[1], operands[2], visible)
        summed, maxima, totals = lax.map(one_head, (jnp.moveaxis(piece_q, 1, 0), jnp.moveaxis(all_k, 1, 0), jnp.moveaxis(all_v, 1, 0)))
        return (fold_group(running, jnp.moveaxis(summed, 0, 1), jnp.moveaxis(maxima, 0, 1), jnp.moveaxis(totals, 0, 1)), None)
    piece_state = lax.scan(piece_group, empty_state(PIECE), jnp.arange(N_KV, dtype=jnp.int32))[0]

    def step_group(running, group_id):
        cache_k = lax.dynamic_slice_in_dim(step_cache_keys, group_id * DCAP_DEV, DCAP_DEV, 1)
        cache_v = lax.dynamic_slice_in_dim(step_cache_values, group_id * DCAP_DEV, DCAP_DEV, 1)
        all_k = jnp.concatenate([cache_k, step_k[:, None]], axis=1)
        all_v = jnp.concatenate([cache_v, step_v[:, None]], axis=1)
        cache_place = group_id * DCAP_DEV + jnp.arange(DCAP_DEV, dtype=jnp.int32)
        visible = jnp.concatenate([cache_place[None, :] < step_lens[:, None], (seq_place // DEC_DEV == group_id)[:, None]], axis=1)
        scores = jnp.einsum('bhcd,bkhcd->bhck', step_q.astype(jnp.float32), all_k.astype(jnp.float32))
        scores = scores * DH ** (-0.5)
        scores = jnp.where(visible[:, None, None, :], scores, -jnp.inf)
        maxima = lax.optimization_barrier(jnp.max(scores, axis=-1))
        weights = jnp.exp(scores - maxima[..., None])
        totals = lax.optimization_barrier(jnp.sum(weights, axis=-1))
        rounded = lax.optimization_barrier(weights.astype(jnp.bfloat16))
        summed = jnp.einsum('bhck,bkhv->bhcv', rounded.astype(jnp.float32), all_v.astype(jnp.float32))
        summed = lax.optimization_barrier(summed.astype(jnp.bfloat16))
        return (fold_group(running, summed, maxima, totals), None)
    step_state = lax.scan(step_group, empty_state(SEQS), jnp.arange(N_KV, dtype=jnp.int32))[0]
    headout = jnp.concatenate([finish(piece_state[1], piece_state[2], mix_ratio, out_gain), finish(step_state[1], step_state[2], mix_ratio, out_gain)], axis=0)
    total_rows = PIECE + SEQS
    per_group = HEADS // N_TP
    grouped = jnp.moveaxis(headout.reshape(total_rows, N_TP, per_group * DV), 1, 0)
    weights = w_out.reshape(N_TP, per_group * DV, D)

    def group_term(operands):
        return jnp.dot(operands[0], operands[1], preferred_element_type=jnp.float32).astype(jnp.bfloat16)
    terms = lax.optimization_barrier(lax.map(group_term, (grouped, weights)))
    mixed = lax.optimization_barrier(jnp.sum(terms.astype(jnp.float32), axis=0)).astype(jnp.bfloat16)
    return (mixed[:PIECE], mixed[PIECE:], piece_k, piece_v, step_k, step_v)
```

```python
import functools
import math

import jax
import jax.numpy as jnp
from jax import lax
from jax.experimental import pallas as pl
from jax.experimental.pallas import tpu as pltpu
from jax.sharding import PartitionSpec as P

EPS = 1e-06
OUT_SCALE = 0.8
MESH = pl.DeviceIdType.MESH
HIDDEN = -1e30


def norm_rows(tokens, in_gain):
    floats = tokens.astype(jnp.float32)
    inv_rms = lax.rsqrt(jnp.mean(floats * floats, axis=-1, keepdims=True) + EPS)
    return (floats * inv_rms * in_gain).astype(jnp.bfloat16)


def project(normed, weight):
    order = tuple(range(1, weight.ndim - 1)) + (0, weight.ndim - 1)
    parts = jnp.transpose(weight, order)
    parts = parts.reshape((-1,) + parts.shape[-2:])
    product = jnp.einsum("nd,gdk->gnk", normed, parts, preferred_element_type=jnp.float32)
    return product.astype(jnp.bfloat16)


def meet(axis, count):
    me = lax.axis_index(axis)
    barrier = pltpu.get_barrier_semaphore()
    for step in range(1, count):
        pl.semaphore_signal(
            barrier, inc=1, device_id={axis: lax.rem(me + step, count)}, device_id_type=MESH
        )
    pl.semaphore_wait(barrier, count - 1)
    return me


def gather_kernel(axis, count, own, everyone, send_sem, recv_sem):
    me = meet(axis, count)
    copies = []
    for step in range(1, count):
        copy = pltpu.make_async_remote_copy(
            src_ref=own,
            dst_ref=everyone.at[me],
            send_sem=send_sem.at[step],
            recv_sem=recv_sem.at[step],
            device_id={axis: lax.rem(me + step, count)},
            device_id_type=MESH,
        )
        copy.start()
        copies.append(copy)
    everyone[me] = own[...]
    for copy in copies:
        copy.wait()


def gather_rows(own, axis, count, collective):
    return pl.pallas_call(
        functools.partial(gather_kernel, axis, count),
        out_shape=jax.ShapeDtypeStruct((count,) + own.shape, own.dtype),
        in_specs=[pl.BlockSpec(memory_space=pltpu.VMEM)],
        out_specs=pl.BlockSpec(memory_space=pltpu.VMEM),
        scratch_shapes=[
            pltpu.SemaphoreType.DMA((count,)),
            pltpu.SemaphoreType.DMA((count,)),
        ],
        compiler_params=pltpu.CompilerParams(collective_id=collective, has_side_effects=True),
        name="gather_rows",
    )(own)


def attend_kernel(rows, dims, q_ref, k_ref, v_ref, fk_ref, fv_ref, bias_ref, own_ref, o_ref, s_ref):
    part = pl.program_id(1)
    owners = q_ref.shape[0]
    scale = dims ** (-0.5)
    fold = scale * math.log2(math.e)
    q = q_ref[:, :rows, :].reshape(owners * rows, dims)
    contract = (((1,), (1,)), ((), ()))
    old = lax.dot_general(q, k_ref[0], contract, preferred_element_type=jnp.float32)
    old = old + bias_ref[...]
    new = lax.dot_general(q, fk_ref[0], contract, preferred_element_type=jnp.float32)
    place = pl.program_id(0) * owners * rows + lax.broadcasted_iota(jnp.int32, new.shape, 0)
    new = jnp.where(own_ref[...] <= place, new, HIDDEN)
    top = jnp.maximum(
        jnp.max(old, axis=1, keepdims=True), jnp.max(new, axis=1, keepdims=True)
    )
    old_w = jnp.exp2((old - top) * fold)
    new_w = jnp.exp2((new - top) * fold)
    total = jnp.sum(old_w, axis=1, keepdims=True) + jnp.sum(new_w, axis=1, keepdims=True)
    summed = jnp.dot(old_w.astype(jnp.bfloat16), v_ref[0], preferred_element_type=jnp.float32)
    summed += jnp.dot(new_w.astype(jnp.bfloat16), fv_ref[0], preferred_element_type=jnp.float32)
    o_ref[...] = summed.astype(jnp.bfloat16).reshape(o_ref.shape)
    parts = pl.num_programs(1)
    lane = lax.broadcasted_iota(jnp.int32, (owners * rows, s_ref.shape[-1]), 1)
    put = jnp.where(lane == part, top * scale, jnp.where(lane == parts + part, total, 0.0))
    put = put.reshape(s_ref.shape)

    @pl.when(part == 0)
    def _():
        s_ref[...] = put

    @pl.when(part != 0)
    def _():
        s_ref[...] += put


def attend(q_all, keys, values, fresh_k, fresh_v, bias, fresh_place, rows):
    count, padded, _ = q_all.shape
    parts, cached, dims = keys.shape
    maps = parts // values.shape[0]
    wide = values.shape[-1]
    owners = math.gcd(count, 2)
    return pl.pallas_call(
        functools.partial(attend_kernel, rows, dims),
        grid=(count // owners, parts),
        in_specs=[
            pl.BlockSpec((owners, padded, dims), lambda i, p: (i, 0, p)),
            pl.BlockSpec((1, cached, dims), lambda i, p: (p, 0, 0)),
            pl.BlockSpec((1, cached, wide), lambda i, p: (p // maps, 0, 0)),
            pl.BlockSpec((1, rows, dims), lambda i, p: (p, 0, 0)),
            pl.BlockSpec((1, rows, wide), lambda i, p: (p // maps, 0, 0)),
            pl.BlockSpec((1, cached), lambda i, p: (0, 0)),
            pl.BlockSpec((1, rows), lambda i, p: (0, 0)),
        ],
        out_specs=[
            pl.BlockSpec((owners, rows, wide), lambda i, p: (i, 0, p)),
            pl.BlockSpec((owners, rows, 128), lambda i, p: (i, 0, 0)),
        ],
        out_shape=[
            jax.ShapeDtypeStruct((count, rows, parts * wide), jnp.bfloat16),
            jax.ShapeDtypeStruct((count, rows, 128), jnp.float32),
        ],
        compiler_params=pltpu.CompilerParams(
            dimension_semantics=("arbitrary", "arbitrary"), vmem_limit_bytes=56 * 1024 * 1024
        ),
        name="attend",
    )(q_all, keys, values, fresh_k, fresh_v, bias, fresh_place)


def mix_maps(first, second, ratio, gain):
    mixed = first - ratio * second
    inv_rms = lax.rsqrt(jnp.mean(mixed * mixed, axis=-1, keepdims=True) + EPS)
    return (mixed * inv_rms * gain * OUT_SCALE).astype(jnp.bfloat16)


def blend(values, tops, totals):
    count = len(values)
    best = functools.reduce(jnp.maximum, tops)
    scales = [jnp.exp(top - best) for top in tops]
    norm = functools.reduce(jnp.add, [scales[g] * totals[g] for g in range(count)])
    total = functools.reduce(jnp.add, [values[g] * scales[g] for g in range(count)])
    return total / norm


def exchange_kernel(
    axis, count, parts, maps, wide, ratio, gain, vals, stats, step, out, all_v, all_s, all_t, send_sem, recv_sem
):
    me = meet(axis, count)
    copies = []
    for turn in range(1, count):
        other = lax.rem(me + turn, count)
        for slot, (mine, theirs) in enumerate(((stats, all_s), (step, all_t), (vals, all_v))):
            copy = pltpu.make_async_remote_copy(
                src_ref=mine.at[other],
                dst_ref=theirs.at[me],
                send_sem=send_sem.at[turn, slot],
                recv_sem=recv_sem.at[turn, slot],
                device_id={axis: other},
                device_id_type=MESH,
            )
            copy.start()
            copies.append(copy)
    all_v[me] = vals[me]
    all_s[me] = stats[me]
    all_t[me] = step[me]
    for copy in copies:
        copy.wait()
    rows = vals.shape[1]
    steps = step.shape[1] // parts
    out[...] = jnp.zeros_like(out)
    tall = math.gcd(rows, 32)

    def chunk(index, carry):
        at = pl.ds(pl.multiple_of(index * tall, tall), tall)
        for head in range(parts // maps):
            maps_out = []
            for part in range(head * maps, head * maps + maps):
                cut = slice(part * wide, part * wide + wide)
                maps_out.append(
                    blend(
                        [all_v[g, at, cut].astype(jnp.float32) for g in range(count)],
                        [all_s[g, at, part : part + 1] for g in range(count)],
                        [all_s[g, at, parts + part : parts + part + 1] for g in range(count)],
                    )
                )
            out[at, head * wide : head * wide + wide] = mix_maps(
                maps_out[0], maps_out[1], ratio[0, head], gain[...]
            )
        return carry

    lax.fori_loop(0, rows // tall, chunk, 0)
    low = out.shape[0] - rows
    for head in range(parts // maps):
        lines = []
        for seq in range(steps):
            maps_out = []
            for part in range(seq * parts + head * maps, seq * parts + head * maps + maps):
                line = [all_t[g, part : part + 1, :] for g in range(count)]
                maps_out.append(
                    blend(
                        [v[:, :wide] for v in line],
                        [v[:, wide : wide + 1] for v in line],
                        [v[:, wide + 1 : wide + 2] for v in line],
                    )
                )
            lines.append(mix_maps(maps_out[0], maps_out[1], ratio[0, head], gain[...]).astype(jnp.float32))
        place = lax.broadcasted_iota(jnp.int32, (low, wide), 0)
        block = jnp.zeros((low, wide), jnp.float32)
        for seq in range(steps):
            block = jnp.where(place == seq, lines[seq], block)
        out[rows:, head * wide : head * wide + wide] = block.astype(jnp.bfloat16)


def exchange(values, stats, step, ratio, gain, axis, count, maps, padded, collective):
    parts = values.shape[-1] // gain.shape[-1]
    wide = gain.shape[-1]
    vmem = pl.BlockSpec(memory_space=pltpu.VMEM)
    return pl.pallas_call(
        functools.partial(exchange_kernel, axis, count, parts, maps, wide),
        out_shape=jax.ShapeDtypeStruct((padded, parts // maps * wide), jnp.bfloat16),
        in_specs=[pl.BlockSpec(memory_space=pltpu.SMEM), vmem, vmem, vmem, vmem],
        out_specs=vmem,
        scratch_shapes=[
            pltpu.VMEM(values.shape, values.dtype),
            pltpu.VMEM(stats.shape, stats.dtype),
            pltpu.VMEM(step.shape, step.dtype),
            pltpu.SemaphoreType.DMA((count, 3)),
            pltpu.SemaphoreType.DMA((count, 3)),
        ],
        compiler_params=pltpu.CompilerParams(
            collective_id=collective, has_side_effects=True, vmem_limit_bytes=56 * 1024 * 1024
        ),
        name="exchange",
    )(ratio, gain, values, stats, step)


def project_out_kernel(axis, count, heads, weight, out, terms, pair, half, far, d_send, d_recv, x_send, x_recv):
    me = lax.axis_index(axis)
    chips = count // 2
    chip, core = me // 2, lax.rem(me, 2)
    meet(axis, count)
    wide = out.shape[1]
    for target in range(count):
        terms[target] = jnp.dot(
            heads[...], weight[:, target * wide : target * wide + wide], preferred_element_type=jnp.float32
        ).astype(jnp.bfloat16)
    near = []
    for turn in range(1, chips + 1):
        there = lax.rem(chip + turn, chips)
        copy = pltpu.make_async_remote_copy(
            src_ref=terms.at[there * 2 + 1 - core],
            dst_ref=pair.at[there],
            send_sem=d_send.at[turn],
            recv_sem=d_recv.at[turn],
            device_id={axis: chip * 2 + 1 - core},
            device_id_type=MESH,
        )
        copy.start()
        near.append(copy)
    away = []
    for turn in range(1, chips + 1):
        near[turn - 1].wait()
        there = lax.rem(chip + turn, chips)
        both = terms[there * 2 + core].astype(jnp.float32) + pair[there].astype(jnp.float32)
        if turn == chips:
            total = both
            for copy in away:
                copy.wait()
            for slot in range(1, chips):
                total = total + far[slot].astype(jnp.float32)
            out[...] = total.astype(jnp.bfloat16)
        else:
            half[turn] = both.astype(jnp.bfloat16)
            copy = pltpu.make_async_remote_copy(
                src_ref=half.at[turn],
                dst_ref=far.at[turn],
                send_sem=x_send.at[turn],
                recv_sem=x_recv.at[turn],
                device_id={axis: there * 2 + core},
                device_id_type=MESH,
            )
            copy.start()
            away.append(copy)


def project_out(heads, weight, axis, count, collective):
    wide = weight.shape[1] // count
    rows = heads.shape[0]
    chips = count // 2
    vmem = pl.BlockSpec(memory_space=pltpu.VMEM)
    return pl.pallas_call(
        functools.partial(project_out_kernel, axis, count),
        out_shape=jax.ShapeDtypeStruct((rows, wide), jnp.bfloat16),
        in_specs=[vmem, vmem],
        out_specs=vmem,
        scratch_shapes=[
            pltpu.VMEM((count, rows, wide), jnp.bfloat16),
            pltpu.VMEM((chips, rows, wide), jnp.bfloat16),
            pltpu.VMEM((chips, rows, wide), jnp.bfloat16),
            pltpu.VMEM((chips, rows, wide), jnp.bfloat16),
            pltpu.SemaphoreType.DMA((chips + 1,)),
            pltpu.SemaphoreType.DMA((chips + 1,)),
            pltpu.SemaphoreType.DMA((chips + 1,)),
            pltpu.SemaphoreType.DMA((chips + 1,)),
        ],
        compiler_params=pltpu.CompilerParams(
            collective_id=collective, has_side_effects=True, vmem_limit_bytes=56 * 1024 * 1024
        ),
        name="project_out",
    )(heads, weight)


def on_device(
    kv_count,
    tp_count,
    piece_tokens,
    step_tokens,
    in_gain,
    w_query,
    w_key,
    w_value,
    w_out,
    mix_ratio,
    out_gain,
    prompt_keys,
    prompt_values,
    step_cache_keys,
    step_cache_values,
    prompt_len,
    step_lens,
):
    kv_place = lax.axis_index("kv")
    piece_dev = piece_tokens.shape[0]
    step_dev = step_tokens.shape[0]
    cache_dev = prompt_keys.shape[0]
    seq_count = step_cache_keys.shape[0]
    seq_cache = step_cache_keys.shape[1]
    heads, maps, dims = w_query.shape[1:]
    wide = w_value.shape[-1]
    parts = heads * maps
    padded = -(-(piece_dev + step_dev) // 16) * 16
    spare = jnp.zeros((padded - piece_dev - step_dev, piece_tokens.shape[1]), jnp.bfloat16)
    all_rows = jnp.concatenate([piece_tokens, step_tokens, spare], axis=0)
    normed = norm_rows(all_rows, in_gain)
    queries = project(normed, w_query)
    key_rows = project(normed, w_key)
    value_rows = project(normed, w_value)
    q_flat = jnp.transpose(queries, (1, 0, 2)).reshape(padded, parts * dims)
    q_all = gather_rows(q_flat, "kv", kv_count, 0)
    end = piece_dev + step_dev

    def rows_of(flat, start, stop, extra):
        return jnp.transpose(flat[:, start:stop], (1, 0, 2)).reshape((stop - start,) + extra)

    piece_k = rows_of(key_rows, 0, piece_dev, (heads, maps, dims))
    step_k = rows_of(key_rows, piece_dev, end, (heads, maps, dims))
    piece_v = rows_of(value_rows, 0, piece_dev, (heads, wide))
    step_v = rows_of(value_rows, piece_dev, end, (heads, wide))
    keys = jnp.transpose(prompt_keys, (1, 2, 0, 3)).reshape(parts, cache_dev, dims)
    values = jnp.transpose(prompt_values, (1, 0, 2))
    cache_ok = kv_place * cache_dev + jnp.arange(cache_dev, dtype=jnp.int32) < prompt_len[0]
    bias = jnp.where(cache_ok, 0.0, HIDDEN)[None, :]
    fresh_place = (kv_place * piece_dev + jnp.arange(piece_dev, dtype=jnp.int32))[None, :]
    piece_sum, piece_stats = attend(
        q_all,
        keys,
        values,
        key_rows[:, :piece_dev],
        value_rows[:, :piece_dev],
        bias,
        fresh_place,
        piece_dev,
    )
    step_q = q_all[:, piece_dev:end].reshape(seq_count, heads, maps, dims)
    own_seq = jnp.arange(seq_count, dtype=jnp.int32) // step_dev == kv_place
    own_k = lax.dynamic_update_slice_in_dim(
        jnp.zeros((seq_count,) + step_k.shape[1:], jnp.bfloat16), step_k, kv_place * step_dev, 0
    )
    own_v = lax.dynamic_update_slice_in_dim(
        jnp.zeros((seq_count,) + step_v.shape[1:], jnp.bfloat16), step_v, kv_place * step_dev, 0
    )
    head_scale = step_q.shape[-1] ** (-0.5)
    cache_scores = (
        jnp.einsum("bhcd,bkhcd->bhck", step_q, step_cache_keys, preferred_element_type=jnp.float32)
        * head_scale
    )
    fresh_scores = (
        jnp.einsum("bhcd,bhcd->bhc", step_q, own_k, preferred_element_type=jnp.float32) * head_scale
    )
    cache_place = kv_place * seq_cache + jnp.arange(seq_cache, dtype=jnp.int32)
    cache_visible = cache_place[None, :] < step_lens[:, None]
    cache_scores = jnp.where(cache_visible[:, None, None, :], cache_scores, -jnp.inf)
    fresh_scores = jnp.where(own_seq[:, None, None], fresh_scores, -jnp.inf)
    step_max = jnp.maximum(jnp.max(cache_scores, axis=-1), fresh_scores)
    cache_weights = jnp.exp(cache_scores - step_max[..., None])
    fresh_weights = jnp.exp(fresh_scores - step_max)
    step_tot = jnp.sum(cache_weights, axis=-1) + fresh_weights
    fresh_rounded = lax.optimization_barrier(fresh_weights.astype(jnp.bfloat16))
    step_acc = jnp.einsum(
        "bhck,bkhv->bhcv",
        cache_weights.astype(jnp.bfloat16),
        step_cache_values,
        preferred_element_type=jnp.float32,
    )
    step_acc = (
        step_acc
        + fresh_rounded.astype(jnp.float32)[..., None] * own_v.astype(jnp.float32)[:, :, None, :]
    )
    step_sum = lax.optimization_barrier(step_acc.astype(jnp.bfloat16))
    message = jnp.concatenate(
        [
            step_sum.astype(jnp.float32),
            step_max[..., None],
            step_tot[..., None],
            jnp.zeros(step_tot.shape + (126,), jnp.float32),
        ],
        axis=-1,
    ).reshape(kv_count, step_dev * parts, wide + 128)
    flat_heads = exchange(
        piece_sum,
        piece_stats,
        message,
        mix_ratio[None, :],
        out_gain[None, :],
        "kv",
        kv_count,
        maps,
        padded,
        1,
    )
    mixed = project_out(flat_heads, w_out.reshape(-1, w_out.shape[-1]), "tp", tp_count, 2)
    return (mixed[:piece_dev], mixed[piece_dev:end], piece_k, piece_v, step_k, step_v)


def solution(mesh):
    in_specs = (
        P("kv", None),
        P("kv", None),
        P(),
        P(None, "tp", None, None),
        P(None, "tp", None, None),
        P(None, "tp", None),
        P("tp", None, None),
        P("tp"),
        P(),
        P("kv", "tp", None, None),
        P("kv", "tp", None),
        P(None, "kv", "tp", None, None),
        P(None, "kv", "tp", None),
        P(),
        P(),
    )
    out_specs = (
        P("kv", "tp"),
        P("kv", "tp"),
        P("kv", "tp", None, None),
        P("kv", "tp", None),
        P("kv", "tp", None, None),
        P("kv", "tp", None),
    )
    return jax.shard_map(
        functools.partial(on_device, mesh.shape["kv"], mesh.shape["tp"]),
        mesh=mesh, in_specs=in_specs, out_specs=out_specs, check_vma=False
    )
```

```python
import functools
import math

import jax
import jax.numpy as jnp
from jax import lax
from jax.experimental import pallas as pl
from jax.experimental.pallas import tpu as pltpu
from jax.sharding import PartitionSpec as P

EPS = 1e-06
OUT_SCALE = 0.8
MESH = pl.DeviceIdType.MESH
HIDDEN = -1e30


def norm_rows(tokens, in_gain):
    floats = tokens.astype(jnp.float32)
    inv_rms = lax.rsqrt(jnp.mean(floats * floats, axis=-1, keepdims=True) + EPS)
    return (floats * inv_rms * in_gain).astype(jnp.bfloat16)


def project(normed, weight):
    order = tuple(range(1, weight.ndim - 1)) + (0, weight.ndim - 1)
    parts = jnp.transpose(weight, order)
    parts = parts.reshape((-1,) + parts.shape[-2:])
    product = jnp.einsum("nd,gdk->gnk", normed, parts, preferred_element_type=jnp.float32)
    return product.astype(jnp.bfloat16)


def meet(axis, count):
    me = lax.axis_index(axis)
    barrier = pltpu.get_barrier_semaphore()
    for step in range(1, count):
        pl.semaphore_signal(
            barrier, inc=1, device_id={axis: lax.rem(me + step, count)}, device_id_type=MESH
        )
    pl.semaphore_wait(barrier, count - 1)
    return me


def grid_of(count):
    across = max(c for c in range(1, count + 1) if count % c == 0 and c * c <= max(count // 2, 1))
    return across, count // across


def gather_kernel(axis, across, along, own, everyone, z_send, z_recv, y_send, y_recv):
    me = meet(axis, across * along)
    z, y = me // across, lax.rem(me, across)

    def hop(way, far):
        step = 1 - 2 * way
        unit = (z - step * far) * across + y
        return pltpu.make_async_remote_copy(
            src_ref=own if far == 0 else everyone.at[unit],
            dst_ref=everyone.at[unit],
            send_sem=z_send.at[way, far],
            recv_sem=z_recv.at[way, far],
            device_id={axis: (z + step) * across + y},
            device_id_type=MESH,
        )

    def arrival(way, far):
        step = 1 - 2 * way
        unit = (z - step * far) * across + y
        return pltpu.make_async_remote_copy(
            src_ref=own,
            dst_ref=everyone.at[unit],
            send_sem=z_send.at[way, far - 1],
            recv_sem=z_recv.at[way, far - 1],
            device_id={axis: (z - step) * across + y},
            device_id_type=MESH,
        )

    def relay(turn, place, source):
        return pltpu.make_async_remote_copy(
            src_ref=source,
            dst_ref=everyone.at[place * across + y],
            send_sem=y_send.at[turn, place],
            recv_sem=y_recv.at[turn, place],
            device_id={axis: z * across + lax.rem(y + turn, across)},
            device_id_type=MESH,
        )

    def can_go(way):
        return z < along - 1 if way == 0 else z > 0

    def has(way, far):
        return z - far >= 0 if way == 0 else z + far < along

    for way in range(2):
        pl.when(can_go(way))(lambda way=way: hop(way, 0).start())
    for turn in range(1, across):
        relay(turn, z, own).start()
    everyone[me] = own[...]
    for far in range(1, along):
        for way in range(2):

            @pl.when(has(way, far))
            def _():
                arrival(way, far).wait_recv()
                if far < along - 1:
                    pl.when(can_go(way))(lambda: hop(way, far).start())
                place = z - far if way == 0 else z + far
                for turn in range(1, across):
                    relay(turn, place, everyone.at[place * across + y]).start()

    for turn in range(1, across):
        came = lax.rem(y + across - turn, across)
        for place in range(along):
            pltpu.make_async_remote_copy(
                src_ref=own,
                dst_ref=everyone.at[place * across + came],
                send_sem=y_send.at[turn, place],
                recv_sem=y_recv.at[turn, place],
                device_id={axis: z * across + came},
                device_id_type=MESH,
            ).wait_recv()
            relay(turn, place, own).wait_send()
    for way in range(2):
        for far in range(along - 1):
            live = can_go(way) if far == 0 else jnp.logical_and(can_go(way), has(way, far))
            pl.when(live)(lambda way=way, far=far: hop(way, far).wait_send())


def gather_rows(own, axis, count, collective):
    across, along = grid_of(count)
    return pl.pallas_call(
        functools.partial(gather_kernel, axis, across, along),
        out_shape=jax.ShapeDtypeStruct((count,) + own.shape, own.dtype),
        in_specs=[pl.BlockSpec(memory_space=pltpu.VMEM)],
        out_specs=pl.BlockSpec(memory_space=pltpu.VMEM),
        scratch_shapes=[
            pltpu.SemaphoreType.DMA((2, along)),
            pltpu.SemaphoreType.DMA((2, along)),
            pltpu.SemaphoreType.DMA((across, along)),
            pltpu.SemaphoreType.DMA((across, along)),
        ],
        compiler_params=pltpu.CompilerParams(collective_id=collective, has_side_effects=True),
        name="gather_rows",
    )(own)


def attend_kernel(rows, dims, q_ref, k_ref, v_ref, fk_ref, fv_ref, bias_ref, own_ref, o_ref, s_ref):
    part = pl.program_id(1)
    owners = q_ref.shape[0]
    scale = dims ** (-0.5)
    fold = scale * math.log2(math.e)
    q = q_ref[:, :rows, :].reshape(owners * rows, dims)
    contract = (((1,), (1,)), ((), ()))
    old = lax.dot_general(q, k_ref[0], contract, preferred_element_type=jnp.float32)
    old = old + bias_ref[...]
    new = lax.dot_general(q, fk_ref[0], contract, preferred_element_type=jnp.float32)
    place = pl.program_id(0) * owners * rows + lax.broadcasted_iota(jnp.int32, new.shape, 0)
    new = jnp.where(own_ref[...] <= place, new, HIDDEN)
    top = jnp.maximum(
        jnp.max(old, axis=1, keepdims=True), jnp.max(new, axis=1, keepdims=True)
    )
    old_w = jnp.exp2((old - top) * fold)
    new_w = jnp.exp2((new - top) * fold)
    total = jnp.sum(old_w, axis=1, keepdims=True) + jnp.sum(new_w, axis=1, keepdims=True)
    summed = jnp.dot(old_w.astype(jnp.bfloat16), v_ref[0], preferred_element_type=jnp.float32)
    summed += jnp.dot(new_w.astype(jnp.bfloat16), fv_ref[0], preferred_element_type=jnp.float32)
    o_ref[...] = (summed / total).astype(jnp.bfloat16).reshape(o_ref.shape)
    lane = lax.broadcasted_iota(jnp.int32, (owners * rows, 128), 1)
    put = jnp.where(lane == part, top * scale + jnp.log(total), 0.0)
    put = jnp.transpose(put)[: s_ref.shape[1]]

    @pl.when(part == 0)
    def _():
        s_ref[0] = put

    @pl.when(part != 0)
    def _():
        s_ref[0] += put


def attend(q_all, keys, values, fresh_k, fresh_v, bias, fresh_place, rows):
    count, padded, _ = q_all.shape
    parts, cached, dims = keys.shape
    maps = parts // values.shape[0]
    wide = values.shape[-1]
    owners = math.gcd(count, 4)
    return pl.pallas_call(
        functools.partial(attend_kernel, rows, dims),
        grid=(count // owners, parts),
        in_specs=[
            pl.BlockSpec((owners, padded, dims), lambda i, p: (i, 0, p)),
            pl.BlockSpec((1, cached, dims), lambda i, p: (p, 0, 0)),
            pl.BlockSpec((1, cached, wide), lambda i, p: (p // maps, 0, 0)),
            pl.BlockSpec((1, rows, dims), lambda i, p: (p, 0, 0)),
            pl.BlockSpec((1, rows, wide), lambda i, p: (p // maps, 0, 0)),
            pl.BlockSpec((1, cached), lambda i, p: (0, 0)),
            pl.BlockSpec((1, rows), lambda i, p: (0, 0)),
        ],
        out_specs=[
            pl.BlockSpec((owners, rows, wide), lambda i, p: (i, 0, p)),
            pl.BlockSpec((1, 8, owners * rows), lambda i, p: (i, 0, 0)),
        ],
        out_shape=[
            jax.ShapeDtypeStruct((count, rows, parts * wide), jnp.bfloat16),
            jax.ShapeDtypeStruct((count // owners, 8, owners * rows), jnp.float32),
        ],
        compiler_params=pltpu.CompilerParams(
            dimension_semantics=("arbitrary", "arbitrary"), vmem_limit_bytes=56 * 1024 * 1024
        ),
        name="attend",
    )(q_all, keys, values, fresh_k, fresh_v, bias, fresh_place)


def shape_head(mixed, gain):
    inv_rms = lax.rsqrt(jnp.mean(mixed * mixed, axis=-1, keepdims=True) + EPS)
    return (mixed * inv_rms * gain * OUT_SCALE).astype(jnp.bfloat16)


def blend(values, tops, totals):
    count = len(values)
    best = functools.reduce(jnp.maximum, tops)
    scales = [jnp.exp(top - best) for top in tops]
    norm = functools.reduce(jnp.add, [scales[g] * totals[g] for g in range(count)])
    total = functools.reduce(jnp.add, [values[g] * scales[g] for g in range(count)])
    return total / norm


def exchange_kernel(
    axis,
    across,
    along,
    parts,
    maps,
    wide,
    ratio,
    gain,
    vals,
    stats,
    step,
    out,
    all_s,
    all_t,
    mine,
    total,
    y_in,
    z_in,
    z_out,
    m_send,
    m_recv,
    y_send,
    y_recv,
    z_send,
    z_recv,
):
    count = across * along
    me = meet(axis, count)
    z, y = me // across, lax.rem(me, across)
    copies = []
    for turn in range(1, count):
        other = lax.rem(me + turn, count)
        for slot, (own, theirs) in enumerate(((stats, all_s.at[me]), (step.at[other], all_t.at[me]))):
            copy = pltpu.make_async_remote_copy(
                src_ref=own,
                dst_ref=theirs,
                send_sem=m_send.at[turn, slot],
                recv_sem=m_recv.at[turn, slot],
                device_id={axis: other},
                device_id_type=MESH,
            )
            copy.start()
            copies.append(copy)
    all_s[me] = stats[...]
    all_t[me] = step[me]
    for copy in copies:
        copy.wait()
    rows = vals.shape[1]
    steps = step.shape[1] // parts
    heads = parts // maps
    blocks, lines, length = stats.shape
    owners = length // rows
    which = lax.broadcasted_iota(jnp.int32, (lines, length), 0)
    sign = jnp.ones((lines, length), jnp.float32)
    for head in range(heads):
        sign = jnp.where(which == head * maps + 1, -ratio[0, head], sign)
    for block in range(blocks):
        best = functools.reduce(jnp.maximum, [all_s[g, block] for g in range(count)])
        norm = functools.reduce(jnp.add, [jnp.exp(all_s[g, block] - best) for g in range(count)])
        share = jnp.exp(stats[block] - best) / norm * sign
        share = jnp.concatenate([share, jnp.zeros((128 - lines, length), jnp.float32)], axis=0)
        column = jnp.transpose(share)
        for owner in range(owners):
            to = block * owners + owner
            c = column[owner * rows : owner * rows + rows]
            for head in range(heads):
                acc = None
                for part in range(head * maps, head * maps + maps):
                    term = c[:, part : part + 1] * vals[to, :, part * wide : part * wide + wide].astype(
                        jnp.float32
                    )
                    acc = term if acc is None else acc + term
                mine[to, :, head * wide : head * wide + wide] = acc.astype(jnp.bfloat16)
    order = sorted(range(along), key=lambda p: (-abs(2 * p - along + 1), -p))

    def over_y(turn, place):
        other = lax.rem(y + turn, across)
        return pltpu.make_async_remote_copy(
            src_ref=mine.at[place * across + other],
            dst_ref=y_in.at[turn, place],
            send_sem=y_send.at[turn, place],
            recv_sem=y_recv.at[turn, place],
            device_id={axis: z * across + other},
            device_id_type=MESH,
        )

    def over_z(way, place):
        return pltpu.make_async_remote_copy(
            src_ref=z_out.at[place],
            dst_ref=z_in.at[way, place],
            send_sem=z_send.at[way, place],
            recv_sem=z_recv.at[way, place],
            device_id={axis: (z + 1 - 2 * way) * across + y},
            device_id_type=MESH,
        )

    def from_z(way, place):
        return pltpu.make_async_remote_copy(
            src_ref=z_out.at[place],
            dst_ref=z_in.at[way, place],
            send_sem=z_send.at[way, place],
            recv_sem=z_recv.at[way, place],
            device_id={axis: (z - 1 + 2 * way) * across + y},
            device_id_type=MESH,
        )

    for place in order:
        for turn in range(1, across):
            over_y(turn, place).start()
    for place in order:
        for turn in range(1, across):
            over_y(turn, place).wait_recv()
        both = mine[place * across + y].astype(jnp.float32)
        for turn in range(1, across):
            both = both + y_in[turn, place].astype(jnp.float32)
        total[...] = both

        @pl.when(z == place)
        def _():
            total_own = both
            mixed_ref = z_out.at[place]
            mixed_ref[...] = total_own.astype(jnp.bfloat16)

        for way in range(2):
            moves = z < place if way == 0 else z > place
            behind = z > 0 if way == 0 else z < along - 1

            @pl.when(moves)
            def _():
                @pl.when(behind)
                def _():
                    from_z(way, place).wait_recv()
                    total[...] += z_in[way, place].astype(jnp.float32)

                z_out[place] = total[...].astype(jnp.bfloat16)
                over_z(way, place).start()

    for place in range(along):

        @pl.when(z == place)
        def _():
            total[...] = z_out[place].astype(jnp.float32)
            for way in range(2):
                if (way == 0 and place > 0) or (way == 1 and place < along - 1):
                    from_z(way, place).wait_recv()
                    total[...] += z_in[way, place].astype(jnp.float32)

        for way in range(2):
            pl.when(z < place if way == 0 else z > place)(
                lambda way=way, place=place: over_z(way, place).wait_send()
            )
        for turn in range(1, across):
            over_y(turn, place).wait_send()
    for head in range(heads):
        cut = slice(head * wide, head * wide + wide)
        out[:rows, cut] = shape_head(total[:, cut], gain[...])
    low = out.shape[0] - rows
    for head in range(heads):
        lines = []
        for seq in range(steps):
            maps_out = []
            for part in range(seq * parts + head * maps, seq * parts + head * maps + maps):
                line = [all_t[g, part : part + 1, :] for g in range(count)]
                maps_out.append(
                    blend(
                        [v[:, :wide] for v in line],
                        [v[:, wide : wide + 1] for v in line],
                        [v[:, wide + 1 : wide + 2] for v in line],
                    )
                )
            lines.append(shape_head(maps_out[0] - ratio[0, head] * maps_out[1], gain[...]).astype(jnp.float32))
        place = lax.broadcasted_iota(jnp.int32, (low, wide), 0)
        block = jnp.zeros((low, wide), jnp.float32)
        for seq in range(steps):
            block = jnp.where(place == seq, lines[seq], block)
        out[rows:, head * wide : head * wide + wide] = block.astype(jnp.bfloat16)


def exchange(values, stats, step, ratio, gain, axis, count, maps, padded, collective):
    across, along = grid_of(count)
    parts = values.shape[-1] // gain.shape[-1]
    wide = gain.shape[-1]
    rows = values.shape[1]
    flat = parts // maps * wide
    vmem = pl.BlockSpec(memory_space=pltpu.VMEM)
    return pl.pallas_call(
        functools.partial(exchange_kernel, axis, across, along, parts, maps, wide),
        out_shape=jax.ShapeDtypeStruct((padded, flat), jnp.bfloat16),
        in_specs=[pl.BlockSpec(memory_space=pltpu.SMEM), vmem, vmem, vmem, vmem],
        out_specs=vmem,
        scratch_shapes=[
            pltpu.VMEM((count,) + stats.shape, stats.dtype),
            pltpu.VMEM(step.shape, step.dtype),
            pltpu.VMEM((count, rows, flat), jnp.bfloat16),
            pltpu.VMEM((rows, flat), jnp.float32),
            pltpu.VMEM((across, along, rows, flat), jnp.bfloat16),
            pltpu.VMEM((2, along, rows, flat), jnp.bfloat16),
            pltpu.VMEM((along, rows, flat), jnp.bfloat16),
            pltpu.SemaphoreType.DMA((count, 2)),
            pltpu.SemaphoreType.DMA((count, 2)),
            pltpu.SemaphoreType.DMA((across, along)),
            pltpu.SemaphoreType.DMA((across, along)),
            pltpu.SemaphoreType.DMA((2, along)),
            pltpu.SemaphoreType.DMA((2, along)),
        ],
        compiler_params=pltpu.CompilerParams(
            collective_id=collective, has_side_effects=True, vmem_limit_bytes=56 * 1024 * 1024
        ),
        name="exchange",
    )(ratio, gain, values, stats, step)


def project_out_kernel(axis, count, heads, weight, out, terms, pair, half, far, d_send, d_recv, x_send, x_recv):
    me = lax.axis_index(axis)
    chips = count // 2
    chip, core = me // 2, lax.rem(me, 2)
    meet(axis, count)
    wide = out.shape[1]
    for target in range(count):
        terms[target] = jnp.dot(
            heads[...], weight[:, target * wide : target * wide + wide], preferred_element_type=jnp.float32
        ).astype(jnp.bfloat16)
    near = []
    for turn in range(1, chips + 1):
        there = lax.rem(chip + turn, chips)
        copy = pltpu.make_async_remote_copy(
            src_ref=terms.at[there * 2 + 1 - core],
            dst_ref=pair.at[there],
            send_sem=d_send.at[turn],
            recv_sem=d_recv.at[turn],
            device_id={axis: chip * 2 + 1 - core},
            device_id_type=MESH,
        )
        copy.start()
        near.append(copy)
    away = []
    for turn in range(1, chips + 1):
        near[turn - 1].wait()
        there = lax.rem(chip + turn, chips)
        both = terms[there * 2 + core].astype(jnp.float32) + pair[there].astype(jnp.float32)
        if turn == chips:
            total = both
            for copy in away:
                copy.wait()
            for slot in range(1, chips):
                total = total + far[slot].astype(jnp.float32)
            out[...] = total.astype(jnp.bfloat16)
        else:
            half[turn] = both.astype(jnp.bfloat16)
            copy = pltpu.make_async_remote_copy(
                src_ref=half.at[turn],
                dst_ref=far.at[turn],
                send_sem=x_send.at[turn],
                recv_sem=x_recv.at[turn],
                device_id={axis: there * 2 + core},
                device_id_type=MESH,
            )
            copy.start()
            away.append(copy)


def project_out(heads, weight, axis, count, collective):
    wide = weight.shape[1] // count
    rows = heads.shape[0]
    chips = count // 2
    vmem = pl.BlockSpec(memory_space=pltpu.VMEM)
    return pl.pallas_call(
        functools.partial(project_out_kernel, axis, count),
        out_shape=jax.ShapeDtypeStruct((rows, wide), jnp.bfloat16),
        in_specs=[vmem, vmem],
        out_specs=vmem,
        scratch_shapes=[
            pltpu.VMEM((count, rows, wide), jnp.bfloat16),
            pltpu.VMEM((chips, rows, wide), jnp.bfloat16),
            pltpu.VMEM((chips, rows, wide), jnp.bfloat16),
            pltpu.VMEM((chips, rows, wide), jnp.bfloat16),
            pltpu.SemaphoreType.DMA((chips + 1,)),
            pltpu.SemaphoreType.DMA((chips + 1,)),
            pltpu.SemaphoreType.DMA((chips + 1,)),
            pltpu.SemaphoreType.DMA((chips + 1,)),
        ],
        compiler_params=pltpu.CompilerParams(
            collective_id=collective, has_side_effects=True, vmem_limit_bytes=56 * 1024 * 1024
        ),
        name="project_out",
    )(heads, weight)


def on_device(
    kv_count,
    tp_count,
    piece_tokens,
    step_tokens,
    in_gain,
    w_query,
    w_key,
    w_value,
    w_out,
    mix_ratio,
    out_gain,
    prompt_keys,
    prompt_values,
    step_cache_keys,
    step_cache_values,
    prompt_len,
    step_lens,
):
    kv_place = lax.axis_index("kv")
    piece_dev = piece_tokens.shape[0]
    step_dev = step_tokens.shape[0]
    cache_dev = prompt_keys.shape[0]
    seq_count = step_cache_keys.shape[0]
    seq_cache = step_cache_keys.shape[1]
    heads, maps, dims = w_query.shape[1:]
    wide = w_value.shape[-1]
    parts = heads * maps
    padded = -(-(piece_dev + step_dev) // 16) * 16
    spare = jnp.zeros((padded - piece_dev - step_dev, piece_tokens.shape[1]), jnp.bfloat16)
    all_rows = jnp.concatenate([piece_tokens, step_tokens, spare], axis=0)
    normed = norm_rows(all_rows, in_gain)
    queries = project(normed, w_query)
    key_rows = project(normed, w_key)
    value_rows = project(normed, w_value)
    q_flat = jnp.transpose(queries, (1, 0, 2)).reshape(padded, parts * dims)
    q_all = gather_rows(q_flat, "kv", kv_count, 0)
    end = piece_dev + step_dev

    def rows_of(flat, start, stop, extra):
        return jnp.transpose(flat[:, start:stop], (1, 0, 2)).reshape((stop - start,) + extra)

    piece_k = rows_of(key_rows, 0, piece_dev, (heads, maps, dims))
    step_k = rows_of(key_rows, piece_dev, end, (heads, maps, dims))
    piece_v = rows_of(value_rows, 0, piece_dev, (heads, wide))
    step_v = rows_of(value_rows, piece_dev, end, (heads, wide))
    keys = jnp.transpose(prompt_keys, (1, 2, 0, 3)).reshape(parts, cache_dev, dims)
    values = jnp.transpose(prompt_values, (1, 0, 2))
    cache_ok = kv_place * cache_dev + jnp.arange(cache_dev, dtype=jnp.int32) < prompt_len[0]
    bias = jnp.where(cache_ok, 0.0, HIDDEN)[None, :]
    fresh_place = (kv_place * piece_dev + jnp.arange(piece_dev, dtype=jnp.int32))[None, :]
    piece_sum, piece_stats = attend(
        q_all,
        keys,
        values,
        key_rows[:, :piece_dev],
        value_rows[:, :piece_dev],
        bias,
        fresh_place,
        piece_dev,
    )
    step_q = q_all[:, piece_dev:end].reshape(seq_count, heads, maps, dims)
    own_seq = jnp.arange(seq_count, dtype=jnp.int32) // step_dev == kv_place
    own_k = lax.dynamic_update_slice_in_dim(
        jnp.zeros((seq_count,) + step_k.shape[1:], jnp.bfloat16), step_k, kv_place * step_dev, 0
    )
    own_v = lax.dynamic_update_slice_in_dim(
        jnp.zeros((seq_count,) + step_v.shape[1:], jnp.bfloat16), step_v, kv_place * step_dev, 0
    )
    head_scale = step_q.shape[-1] ** (-0.5)
    cache_scores = (
        jnp.einsum("bhcd,bkhcd->bhck", step_q, step_cache_keys, preferred_element_type=jnp.float32)
        * head_scale
    )
    fresh_scores = (
        jnp.einsum("bhcd,bhcd->bhc", step_q, own_k, preferred_element_type=jnp.float32) * head_scale
    )
    cache_place = kv_place * seq_cache + jnp.arange(seq_cache, dtype=jnp.int32)
    cache_visible = cache_place[None, :] < step_lens[:, None]
    cache_scores = jnp.where(cache_visible[:, None, None, :], cache_scores, -jnp.inf)
    fresh_scores = jnp.where(own_seq[:, None, None], fresh_scores, -jnp.inf)
    step_max = jnp.maximum(jnp.max(cache_scores, axis=-1), fresh_scores)
    cache_weights = jnp.exp(cache_scores - step_max[..., None])
    fresh_weights = jnp.exp(fresh_scores - step_max)
    step_tot = jnp.sum(cache_weights, axis=-1) + fresh_weights
    fresh_rounded = lax.optimization_barrier(fresh_weights.astype(jnp.bfloat16))
    step_acc = jnp.einsum(
        "bhck,bkhv->bhcv",
        cache_weights.astype(jnp.bfloat16),
        step_cache_values,
        preferred_element_type=jnp.float32,
    )
    step_acc = (
        step_acc
        + fresh_rounded.astype(jnp.float32)[..., None] * own_v.astype(jnp.float32)[:, :, None, :]
    )
    step_sum = lax.optimization_barrier(step_acc.astype(jnp.bfloat16))
    message = jnp.concatenate(
        [
            step_sum.astype(jnp.float32),
            step_max[..., None],
            step_tot[..., None],
            jnp.zeros(step_tot.shape + (126,), jnp.float32),
        ],
        axis=-1,
    ).reshape(kv_count, step_dev * parts, wide + 128)
    flat_heads = exchange(
        piece_sum,
        piece_stats,
        message,
        mix_ratio[None, :],
        out_gain[None, :],
        "kv",
        kv_count,
        maps,
        padded,
        1,
    )
    mixed = project_out(flat_heads, w_out.reshape(-1, w_out.shape[-1]), "tp", tp_count, 2)
    return (mixed[:piece_dev], mixed[piece_dev:end], piece_k, piece_v, step_k, step_v)


def solution(mesh):
    in_specs = (
        P("kv", None),
        P("kv", None),
        P(),
        P(None, "tp", None, None),
        P(None, "tp", None, None),
        P(None, "tp", None),
        P("tp", None, None),
        P("tp"),
        P(),
        P("kv", "tp", None, None),
        P("kv", "tp", None),
        P(None, "kv", "tp", None, None),
        P(None, "kv", "tp", None),
        P(),
        P(),
    )
    out_specs = (
        P("kv", "tp"),
        P("kv", "tp"),
        P("kv", "tp", None, None),
        P("kv", "tp", None),
        P("kv", "tp", None, None),
        P("kv", "tp", None),
    )
    return jax.shard_map(
        functools.partial(on_device, mesh.shape["kv"], mesh.shape["tp"]),
        mesh=mesh, in_specs=in_specs, out_specs=out_specs, check_vma=False
    )
```

```python
import functools
import math

import jax
import jax.numpy as jnp
from jax import lax
from jax.experimental import pallas as pl
from jax.experimental.pallas import tpu as pltpu
from jax.sharding import PartitionSpec as P

EPS = 1e-06
OUT_SCALE = 0.8
MESH = pl.DeviceIdType.MESH
HIDDEN = -1e30


def norm_rows(tokens, in_gain):
    floats = tokens.astype(jnp.float32)
    inv_rms = lax.rsqrt(jnp.mean(floats * floats, axis=-1, keepdims=True) + EPS)
    return (floats * inv_rms * in_gain).astype(jnp.bfloat16)


def project(normed, weight):
    order = tuple(range(1, weight.ndim - 1)) + (0, weight.ndim - 1)
    parts = jnp.transpose(weight, order)
    parts = parts.reshape((-1,) + parts.shape[-2:])
    product = jnp.einsum("nd,gdk->gnk", normed, parts, preferred_element_type=jnp.float32)
    return product.astype(jnp.bfloat16)


def meet(axis, count):
    me = lax.axis_index(axis)
    barrier = pltpu.get_barrier_semaphore()
    for step in range(1, count):
        pl.semaphore_signal(
            barrier, inc=1, device_id={axis: lax.rem(me + step, count)}, device_id_type=MESH
        )
    pl.semaphore_wait(barrier, count - 1)
    return me


def grid_of(count):
    across = max(c for c in range(1, count + 1) if count % c == 0 and c * c <= max(count // 2, 1))
    return across, count // across


def gather_kernel(axis, across, along, own, everyone, z_send, z_recv, y_send, y_recv):
    me = meet(axis, across * along)
    z, y = me // across, lax.rem(me, across)

    def hop(way, far):
        step = 1 - 2 * way
        unit = (z - step * far) * across + y
        return pltpu.make_async_remote_copy(
            src_ref=own if far == 0 else everyone.at[unit],
            dst_ref=everyone.at[unit],
            send_sem=z_send.at[way, far],
            recv_sem=z_recv.at[way, far],
            device_id={axis: (z + step) * across + y},
            device_id_type=MESH,
        )

    def arrival(way, far):
        step = 1 - 2 * way
        unit = (z - step * far) * across + y
        return pltpu.make_async_remote_copy(
            src_ref=own,
            dst_ref=everyone.at[unit],
            send_sem=z_send.at[way, far - 1],
            recv_sem=z_recv.at[way, far - 1],
            device_id={axis: (z - step) * across + y},
            device_id_type=MESH,
        )

    def relay(turn, place, source):
        return pltpu.make_async_remote_copy(
            src_ref=source,
            dst_ref=everyone.at[place * across + y],
            send_sem=y_send.at[turn, place],
            recv_sem=y_recv.at[turn, place],
            device_id={axis: z * across + lax.rem(y + turn, across)},
            device_id_type=MESH,
        )

    def can_go(way):
        return z < along - 1 if way == 0 else z > 0

    def has(way, far):
        return z - far >= 0 if way == 0 else z + far < along

    for way in range(2):
        pl.when(can_go(way))(lambda way=way: hop(way, 0).start())
    for turn in range(1, across):
        relay(turn, z, own).start()
    everyone[me] = own[...]
    for far in range(1, along):
        for way in range(2):

            @pl.when(has(way, far))
            def _():
                arrival(way, far).wait_recv()
                if far < along - 1:
                    pl.when(can_go(way))(lambda: hop(way, far).start())
                place = z - far if way == 0 else z + far
                for turn in range(1, across):
                    relay(turn, place, everyone.at[place * across + y]).start()

    for turn in range(1, across):
        came = lax.rem(y + across - turn, across)
        for place in range(along):
            pltpu.make_async_remote_copy(
                src_ref=own,
                dst_ref=everyone.at[place * across + came],
                send_sem=y_send.at[turn, place],
                recv_sem=y_recv.at[turn, place],
                device_id={axis: z * across + came},
                device_id_type=MESH,
            ).wait_recv()
            relay(turn, place, own).wait_send()
    for way in range(2):
        for far in range(along - 1):
            live = can_go(way) if far == 0 else jnp.logical_and(can_go(way), has(way, far))
            pl.when(live)(lambda way=way, far=far: hop(way, far).wait_send())


def gather_rows(own, axis, count, collective):
    across, along = grid_of(count)
    return pl.pallas_call(
        functools.partial(gather_kernel, axis, across, along),
        out_shape=jax.ShapeDtypeStruct((count,) + own.shape, own.dtype),
        in_specs=[pl.BlockSpec(memory_space=pltpu.VMEM)],
        out_specs=pl.BlockSpec(memory_space=pltpu.VMEM),
        scratch_shapes=[
            pltpu.SemaphoreType.DMA((2, along)),
            pltpu.SemaphoreType.DMA((2, along)),
            pltpu.SemaphoreType.DMA((across, along)),
            pltpu.SemaphoreType.DMA((across, along)),
        ],
        compiler_params=pltpu.CompilerParams(collective_id=collective, has_side_effects=True),
        name="gather_rows",
    )(own)


def attend_kernel(rows, dims, q_ref, k_ref, v_ref, fk_ref, fv_ref, bias_ref, own_ref, o_ref, s_ref):
    part = pl.program_id(1)
    owners = q_ref.shape[0]
    scale = dims ** (-0.5)
    fold = scale * math.log2(math.e)
    some = math.gcd(owners, 2)
    logs = []
    for at in range(0, owners, some):
        q = q_ref[at : at + some, :rows, :].reshape(some * rows, dims)
        contract = (((1,), (1,)), ((), ()))
        old = lax.dot_general(q, k_ref[0], contract, preferred_element_type=jnp.float32)
        old = old + bias_ref[...]
        new = lax.dot_general(q, fk_ref[0], contract, preferred_element_type=jnp.float32)
        place = (pl.program_id(0) * owners + at) * rows + lax.broadcasted_iota(jnp.int32, new.shape, 0)
        new = jnp.where(own_ref[...] <= place, new, HIDDEN)
        top = jnp.maximum(
            jnp.max(old, axis=1, keepdims=True), jnp.max(new, axis=1, keepdims=True)
        )
        old_w = jnp.exp2((old - top) * fold)
        new_w = jnp.exp2((new - top) * fold)
        total = jnp.sum(old_w, axis=1, keepdims=True) + jnp.sum(new_w, axis=1, keepdims=True)
        summed = jnp.dot(old_w.astype(jnp.bfloat16), v_ref[0], preferred_element_type=jnp.float32)
        summed += jnp.dot(new_w.astype(jnp.bfloat16), fv_ref[0], preferred_element_type=jnp.float32)
        o_ref[at : at + some] = (summed / total).astype(jnp.bfloat16).reshape(some, rows, -1)
        logs.append(top * scale + jnp.log(total))
    lane = lax.broadcasted_iota(jnp.int32, (owners * rows, 128), 1)
    put = jnp.where(lane == part, jnp.concatenate(logs, axis=0), 0.0)
    put = jnp.transpose(put)[: s_ref.shape[1]]

    @pl.when(part == 0)
    def _():
        s_ref[0] = put

    @pl.when(part != 0)
    def _():
        s_ref[0] += put


def attend(q_all, keys, values, fresh_k, fresh_v, bias, fresh_place, rows):
    count, padded, _ = q_all.shape
    parts, cached, dims = keys.shape
    maps = parts // values.shape[0]
    wide = values.shape[-1]
    owners = math.gcd(count, 4)
    return pl.pallas_call(
        functools.partial(attend_kernel, rows, dims),
        grid=(count // owners, parts),
        in_specs=[
            pl.BlockSpec((owners, padded, dims), lambda i, p: (i, 0, p)),
            pl.BlockSpec((1, cached, dims), lambda i, p: (p, 0, 0)),
            pl.BlockSpec((1, cached, wide), lambda i, p: (p // maps, 0, 0)),
            pl.BlockSpec((1, rows, dims), lambda i, p: (p, 0, 0)),
            pl.BlockSpec((1, rows, wide), lambda i, p: (p // maps, 0, 0)),
            pl.BlockSpec((1, cached), lambda i, p: (0, 0)),
            pl.BlockSpec((1, rows), lambda i, p: (0, 0)),
        ],
        out_specs=[
            pl.BlockSpec((owners, rows, wide), lambda i, p: (i, 0, p)),
            pl.BlockSpec((1, 8, owners * rows), lambda i, p: (i, 0, 0)),
        ],
        out_shape=[
            jax.ShapeDtypeStruct((count, rows, parts * wide), jnp.bfloat16),
            jax.ShapeDtypeStruct((count // owners, 8, owners * rows), jnp.float32),
        ],
        compiler_params=pltpu.CompilerParams(
            dimension_semantics=("arbitrary", "arbitrary"), vmem_limit_bytes=56 * 1024 * 1024
        ),
        name="attend",
    )(q_all, keys, values, fresh_k, fresh_v, bias, fresh_place)


def shape_head(mixed, gain):
    inv_rms = lax.rsqrt(jnp.mean(mixed * mixed, axis=-1, keepdims=True) + EPS)
    return (mixed * inv_rms * gain * OUT_SCALE).astype(jnp.bfloat16)


def blend(values, tops, totals):
    count = len(values)
    best = functools.reduce(jnp.maximum, tops)
    scales = [jnp.exp(top - best) for top in tops]
    norm = functools.reduce(jnp.add, [scales[g] * totals[g] for g in range(count)])
    total = functools.reduce(jnp.add, [values[g] * scales[g] for g in range(count)])
    return total / norm


def exchange_kernel(
    axis,
    across,
    along,
    parts,
    maps,
    wide,
    ratio,
    gain,
    vals,
    stats,
    step,
    out,
    all_s,
    all_t,
    mine,
    total,
    y_in,
    z_in,
    z_out,
    m_send,
    m_recv,
    y_send,
    y_recv,
    z_send,
    z_recv,
):
    count = across * along
    me = meet(axis, count)
    z, y = me // across, lax.rem(me, across)
    copies = []
    for turn in range(1, count):
        other = lax.rem(me + turn, count)
        for slot, (own, theirs) in enumerate(((stats, all_s.at[me]), (step.at[other], all_t.at[me]))):
            copy = pltpu.make_async_remote_copy(
                src_ref=own,
                dst_ref=theirs,
                send_sem=m_send.at[turn, slot],
                recv_sem=m_recv.at[turn, slot],
                device_id={axis: other},
                device_id_type=MESH,
            )
            copy.start()
            copies.append(copy)
    all_s[me] = stats[...]
    all_t[me] = step[me]
    for copy in copies:
        copy.wait()
    rows = vals.shape[1]
    steps = step.shape[1] // parts
    heads = parts // maps
    blocks, lines, length = stats.shape
    owners = length // rows
    which = lax.broadcasted_iota(jnp.int32, (lines, length), 0)
    sign = jnp.ones((lines, length), jnp.float32)
    for head in range(heads):
        sign = jnp.where(which == head * maps + 1, -ratio[0, head], sign)
    for block in range(blocks):
        best = functools.reduce(jnp.maximum, [all_s[g, block] for g in range(count)])
        norm = functools.reduce(jnp.add, [jnp.exp(all_s[g, block] - best) for g in range(count)])
        share = jnp.exp(stats[block] - best) / norm * sign
        share = jnp.concatenate([share, jnp.zeros((128 - lines, length), jnp.float32)], axis=0)
        column = jnp.transpose(share)
        for owner in range(owners):
            to = block * owners + owner
            c = column[owner * rows : owner * rows + rows]
            for head in range(heads):
                acc = None
                for part in range(head * maps, head * maps + maps):
                    term = c[:, part : part + 1] * vals[to, :, part * wide : part * wide + wide].astype(
                        jnp.float32
                    )
                    acc = term if acc is None else acc + term
                mine[to, :, head * wide : head * wide + wide] = acc.astype(jnp.bfloat16)
    order = sorted(range(along), key=lambda p: (-abs(2 * p - along + 1), -p))

    def over_y(turn, place):
        other = lax.rem(y + turn, across)
        return pltpu.make_async_remote_copy(
            src_ref=mine.at[place * across + other],
            dst_ref=y_in.at[turn, place],
            send_sem=y_send.at[turn, place],
            recv_sem=y_recv.at[turn, place],
            device_id={axis: z * across + other},
            device_id_type=MESH,
        )

    def over_z(way, place):
        return pltpu.make_async_remote_copy(
            src_ref=z_out.at[place],
            dst_ref=z_in.at[way, place],
            send_sem=z_send.at[way, place],
            recv_sem=z_recv.at[way, place],
            device_id={axis: (z + 1 - 2 * way) * across + y},
            device_id_type=MESH,
        )

    def from_z(way, place):
        return pltpu.make_async_remote_copy(
            src_ref=z_out.at[place],
            dst_ref=z_in.at[way, place],
            send_sem=z_send.at[way, place],
            recv_sem=z_recv.at[way, place],
            device_id={axis: (z - 1 + 2 * way) * across + y},
            device_id_type=MESH,
        )

    for place in order:
        for turn in range(1, across):
            over_y(turn, place).start()
    for place in order:
        for turn in range(1, across):
            over_y(turn, place).wait_recv()
        both = mine[place * across + y].astype(jnp.float32)
        for turn in range(1, across):
            both = both + y_in[turn, place].astype(jnp.float32)
        total[...] = both

        @pl.when(z == place)
        def _():
            total_own = both
            mixed_ref = z_out.at[place]
            mixed_ref[...] = total_own.astype(jnp.bfloat16)

        for way in range(2):
            moves = z < place if way == 0 else z > place
            behind = z > 0 if way == 0 else z < along - 1

            @pl.when(moves)
            def _():
                @pl.when(behind)
                def _():
                    from_z(way, place).wait_recv()
                    total[...] += z_in[way, place].astype(jnp.float32)

                z_out[place] = total[...].astype(jnp.bfloat16)
                over_z(way, place).start()

    for place in range(along):

        @pl.when(z == place)
        def _():
            total[...] = z_out[place].astype(jnp.float32)
            for way in range(2):
                if (way == 0 and place > 0) or (way == 1 and place < along - 1):
                    from_z(way, place).wait_recv()
                    total[...] += z_in[way, place].astype(jnp.float32)

        for way in range(2):
            pl.when(z < place if way == 0 else z > place)(
                lambda way=way, place=place: over_z(way, place).wait_send()
            )
        for turn in range(1, across):
            over_y(turn, place).wait_send()
    for head in range(heads):
        cut = slice(head * wide, head * wide + wide)
        out[:rows, cut] = shape_head(total[:, cut], gain[...])
    low = out.shape[0] - rows
    for head in range(heads):
        lines = []
        for seq in range(steps):
            maps_out = []
            for part in range(seq * parts + head * maps, seq * parts + head * maps + maps):
                line = [all_t[g, part : part + 1, :] for g in range(count)]
                maps_out.append(
                    blend(
                        [v[:, :wide] for v in line],
                        [v[:, wide : wide + 1] for v in line],
                        [v[:, wide + 1 : wide + 2] for v in line],
                    )
                )
            lines.append(shape_head(maps_out[0] - ratio[0, head] * maps_out[1], gain[...]).astype(jnp.float32))
        place = lax.broadcasted_iota(jnp.int32, (low, wide), 0)
        block = jnp.zeros((low, wide), jnp.float32)
        for seq in range(steps):
            block = jnp.where(place == seq, lines[seq], block)
        out[rows:, head * wide : head * wide + wide] = block.astype(jnp.bfloat16)


def exchange(values, stats, step, ratio, gain, axis, count, maps, padded, collective):
    across, along = grid_of(count)
    parts = values.shape[-1] // gain.shape[-1]
    wide = gain.shape[-1]
    rows = values.shape[1]
    flat = parts // maps * wide
    vmem = pl.BlockSpec(memory_space=pltpu.VMEM)
    return pl.pallas_call(
        functools.partial(exchange_kernel, axis, across, along, parts, maps, wide),
        out_shape=jax.ShapeDtypeStruct((padded, flat), jnp.bfloat16),
        in_specs=[pl.BlockSpec(memory_space=pltpu.SMEM), vmem, vmem, vmem, vmem],
        out_specs=vmem,
        scratch_shapes=[
            pltpu.VMEM((count,) + stats.shape, stats.dtype),
            pltpu.VMEM(step.shape, step.dtype),
            pltpu.VMEM((count, rows, flat), jnp.bfloat16),
            pltpu.VMEM((rows, flat), jnp.float32),
            pltpu.VMEM((across, along, rows, flat), jnp.bfloat16),
            pltpu.VMEM((2, along, rows, flat), jnp.bfloat16),
            pltpu.VMEM((along, rows, flat), jnp.bfloat16),
            pltpu.SemaphoreType.DMA((count, 2)),
            pltpu.SemaphoreType.DMA((count, 2)),
            pltpu.SemaphoreType.DMA((across, along)),
            pltpu.SemaphoreType.DMA((across, along)),
            pltpu.SemaphoreType.DMA((2, along)),
            pltpu.SemaphoreType.DMA((2, along)),
        ],
        compiler_params=pltpu.CompilerParams(
            collective_id=collective, has_side_effects=True, vmem_limit_bytes=56 * 1024 * 1024
        ),
        name="exchange",
    )(ratio, gain, values, stats, step)


def project_out_kernel(axis, count, heads, weight, out, terms, pair, half, far, d_send, d_recv, x_send, x_recv):
    me = lax.axis_index(axis)
    chips = count // 2
    chip, core = me // 2, lax.rem(me, 2)
    meet(axis, count)
    wide = out.shape[1]
    for target in range(count):
        terms[target] = jnp.dot(
            heads[...], weight[:, target * wide : target * wide + wide], preferred_element_type=jnp.float32
        ).astype(jnp.bfloat16)
    near = []
    for turn in range(1, chips + 1):
        there = lax.rem(chip + turn, chips)
        copy = pltpu.make_async_remote_copy(
            src_ref=terms.at[there * 2 + 1 - core],
            dst_ref=pair.at[there],
            send_sem=d_send.at[turn],
            recv_sem=d_recv.at[turn],
            device_id={axis: chip * 2 + 1 - core},
            device_id_type=MESH,
        )
        copy.start()
        near.append(copy)
    away = []
    for turn in range(1, chips + 1):
        near[turn - 1].wait()
        there = lax.rem(chip + turn, chips)
        both = terms[there * 2 + core].astype(jnp.float32) + pair[there].astype(jnp.float32)
        if turn == chips:
            total = both
            for copy in away:
                copy.wait()
            for slot in range(1, chips):
                total = total + far[slot].astype(jnp.float32)
            out[...] = total.astype(jnp.bfloat16)
        else:
            half[turn] = both.astype(jnp.bfloat16)
            copy = pltpu.make_async_remote_copy(
                src_ref=half.at[turn],
                dst_ref=far.at[turn],
                send_sem=x_send.at[turn],
                recv_sem=x_recv.at[turn],
                device_id={axis: there * 2 + core},
                device_id_type=MESH,
            )
            copy.start()
            away.append(copy)


def project_out(heads, weight, axis, count, collective):
    wide = weight.shape[1] // count
    rows = heads.shape[0]
    chips = count // 2
    vmem = pl.BlockSpec(memory_space=pltpu.VMEM)
    return pl.pallas_call(
        functools.partial(project_out_kernel, axis, count),
        out_shape=jax.ShapeDtypeStruct((rows, wide), jnp.bfloat16),
        in_specs=[vmem, vmem],
        out_specs=vmem,
        scratch_shapes=[
            pltpu.VMEM((count, rows, wide), jnp.bfloat16),
            pltpu.VMEM((chips, rows, wide), jnp.bfloat16),
            pltpu.VMEM((chips, rows, wide), jnp.bfloat16),
            pltpu.VMEM((chips, rows, wide), jnp.bfloat16),
            pltpu.SemaphoreType.DMA((chips + 1,)),
            pltpu.SemaphoreType.DMA((chips + 1,)),
            pltpu.SemaphoreType.DMA((chips + 1,)),
            pltpu.SemaphoreType.DMA((chips + 1,)),
        ],
        compiler_params=pltpu.CompilerParams(
            collective_id=collective, has_side_effects=True, vmem_limit_bytes=56 * 1024 * 1024
        ),
        name="project_out",
    )(heads, weight)


def on_device(
    kv_count,
    tp_count,
    piece_tokens,
    step_tokens,
    in_gain,
    w_query,
    w_key,
    w_value,
    w_out,
    mix_ratio,
    out_gain,
    prompt_keys,
    prompt_values,
    step_cache_keys,
    step_cache_values,
    prompt_len,
    step_lens,
):
    kv_place = lax.axis_index("kv")
    piece_dev = piece_tokens.shape[0]
    step_dev = step_tokens.shape[0]
    cache_dev = prompt_keys.shape[0]
    seq_count = step_cache_keys.shape[0]
    seq_cache = step_cache_keys.shape[1]
    heads, maps, dims = w_query.shape[1:]
    wide = w_value.shape[-1]
    parts = heads * maps
    padded = -(-(piece_dev + step_dev) // 16) * 16
    spare = jnp.zeros((padded - piece_dev - step_dev, piece_tokens.shape[1]), jnp.bfloat16)
    all_rows = jnp.concatenate([piece_tokens, step_tokens, spare], axis=0)
    normed = norm_rows(all_rows, in_gain)
    queries = project(normed, w_query)
    key_rows = project(normed, w_key)
    value_rows = project(normed, w_value)
    q_flat = jnp.transpose(queries, (1, 0, 2)).reshape(padded, parts * dims)
    q_all = gather_rows(q_flat, "kv", kv_count, 0)
    end = piece_dev + step_dev

    def rows_of(flat, start, stop, extra):
        return jnp.transpose(flat[:, start:stop], (1, 0, 2)).reshape((stop - start,) + extra)

    piece_k = rows_of(key_rows, 0, piece_dev, (heads, maps, dims))
    step_k = rows_of(key_rows, piece_dev, end, (heads, maps, dims))
    piece_v = rows_of(value_rows, 0, piece_dev, (heads, wide))
    step_v = rows_of(value_rows, piece_dev, end, (heads, wide))
    keys = jnp.transpose(prompt_keys, (1, 2, 0, 3)).reshape(parts, cache_dev, dims)
    values = jnp.transpose(prompt_values, (1, 0, 2))
    cache_ok = kv_place * cache_dev + jnp.arange(cache_dev, dtype=jnp.int32) < prompt_len[0]
    bias = jnp.where(cache_ok, 0.0, HIDDEN)[None, :]
    fresh_place = (kv_place * piece_dev + jnp.arange(piece_dev, dtype=jnp.int32))[None, :]
    piece_sum, piece_stats = attend(
        q_all,
        keys,
        values,
        key_rows[:, :piece_dev],
        value_rows[:, :piece_dev],
        bias,
        fresh_place,
        piece_dev,
    )
    step_q = q_all[:, piece_dev:end].reshape(seq_count, heads, maps, dims)
    own_seq = jnp.arange(seq_count, dtype=jnp.int32) // step_dev == kv_place
    own_k = lax.dynamic_update_slice_in_dim(
        jnp.zeros((seq_count,) + step_k.shape[1:], jnp.bfloat16), step_k, kv_place * step_dev, 0
    )
    own_v = lax.dynamic_update_slice_in_dim(
        jnp.zeros((seq_count,) + step_v.shape[1:], jnp.bfloat16), step_v, kv_place * step_dev, 0
    )
    head_scale = step_q.shape[-1] ** (-0.5)
    cache_scores = (
        jnp.einsum("bhcd,bkhcd->bhck", step_q, step_cache_keys, preferred_element_type=jnp.float32)
        * head_scale
    )
    fresh_scores = (
        jnp.einsum("bhcd,bhcd->bhc", step_q, own_k, preferred_element_type=jnp.float32) * head_scale
    )
    cache_place = kv_place * seq_cache + jnp.arange(seq_cache, dtype=jnp.int32)
    cache_visible = cache_place[None, :] < step_lens[:, None]
    cache_scores = jnp.where(cache_visible[:, None, None, :], cache_scores, -jnp.inf)
    fresh_scores = jnp.where(own_seq[:, None, None], fresh_scores, -jnp.inf)
    step_max = jnp.maximum(jnp.max(cache_scores, axis=-1), fresh_scores)
    cache_weights = jnp.exp(cache_scores - step_max[..., None])
    fresh_weights = jnp.exp(fresh_scores - step_max)
    step_tot = jnp.sum(cache_weights, axis=-1) + fresh_weights
    fresh_rounded = lax.optimization_barrier(fresh_weights.astype(jnp.bfloat16))
    step_acc = jnp.einsum(
        "bhck,bkhv->bhcv",
        cache_weights.astype(jnp.bfloat16),
        step_cache_values,
        preferred_element_type=jnp.float32,
    )
    step_acc = (
        step_acc
        + fresh_rounded.astype(jnp.float32)[..., None] * own_v.astype(jnp.float32)[:, :, None, :]
    )
    step_sum = lax.optimization_barrier(step_acc.astype(jnp.bfloat16))
    message = jnp.concatenate(
        [
            step_sum.astype(jnp.float32),
            step_max[..., None],
            step_tot[..., None],
            jnp.zeros(step_tot.shape + (126,), jnp.float32),
        ],
        axis=-1,
    ).reshape(kv_count, step_dev * parts, wide + 128)
    flat_heads = exchange(
        piece_sum,
        piece_stats,
        message,
        mix_ratio[None, :],
        out_gain[None, :],
        "kv",
        kv_count,
        maps,
        padded,
        1,
    )
    mixed = project_out(flat_heads, w_out.reshape(-1, w_out.shape[-1]), "tp", tp_count, 2)
    return (mixed[:piece_dev], mixed[piece_dev:end], piece_k, piece_v, step_k, step_v)


def solution(mesh):
    in_specs = (
        P("kv", None),
        P("kv", None),
        P(),
        P(None, "tp", None, None),
        P(None, "tp", None, None),
        P(None, "tp", None),
        P("tp", None, None),
        P("tp"),
        P(),
        P("kv", "tp", None, None),
        P("kv", "tp", None),
        P(None, "kv", "tp", None, None),
        P(None, "kv", "tp", None),
        P(),
        P(),
    )
    out_specs = (
        P("kv", "tp"),
        P("kv", "tp"),
        P("kv", "tp", None, None),
        P("kv", "tp", None),
        P("kv", "tp", None, None),
        P("kv", "tp", None),
    )
    return jax.shard_map(
        functools.partial(on_device, mesh.shape["kv"], mesh.shape["tp"]),
        mesh=mesh, in_specs=in_specs, out_specs=out_specs, check_vma=False
    )
```
